32 devices in a mesh: sp: 8 (over z, x), tp: 4 (over y, core).
Axes of the slice: x: 2, y: 2, z: 4, core: 2. Of those that a mesh axis runs over, the one named last changes fastest.
Arguments:
- layer_input: bfloat16 [1024, 2048], P('sp'), may hold values from -6 to 6
- out_cot: bfloat16 [1024, 2048], P('sp'), may hold values from -6 to 6
- routes: int32 [1024, 2], P('sp'), may hold values from 0 to 7, all different within a row; in each aligned block of 128 rows (0 to 127, 128 to 255, ...) at most 64 rows name the same one
- route_weights: float32 [1024, 2], P('sp'), may hold values from 0.2 to 1
- gate_weights: bfloat16 [8, 2048, 1024], P('sp', None, 'tp'), may hold values from -0.125 to 0.125
- up_weights: bfloat16 [8, 2048, 1024], P('sp', None, 'tp'), may hold values from -0.125 to 0.125
- down_weights: bfloat16 [8, 1024, 2048], P('sp', 'tp'), may hold values from -0.1875 to 0.1875
- out_proj: bfloat16 [2048, 2048], P(None, 'tp'), may hold values from -0.125 to 0.125
- queries: bfloat16 [1024, 2048], P('sp', 'tp'), may hold values from -6 to 6
- keys: bfloat16 [1024, 2048], P('sp', 'tp'), may hold values from -6 to 6
- values: bfloat16 [1024, 2048], P('sp', 'tp'), may hold values from -6 to 6
- mixer_out: bfloat16 [1024, 2048], P('sp', 'tp'), may hold values from -6 to 6
- entry_states: float32 [8, 32, 64, 64], P('sp', 'tp'), may hold values from -6 to 6
Outputs:
- grad_gate: bfloat16 [8, 2048, 1024], P('sp', None, 'tp')
- grad_up: bfloat16 [8, 2048, 1024], P('sp', None, 'tp')
- grad_down: bfloat16 [8, 1024, 2048], P('sp', 'tp')
- grad_proj: float32 [2048, 2048], P('sp', 'tp')
- grad_queries: bfloat16 [1024, 2048], P('sp', 'tp')
- grad_keys: bfloat16 [1024, 2048], P('sp', 'tp')
- grad_values: bfloat16 [1024, 2048], P('sp', 'tp')
The draws below stay inside these ranges and needn't reach their ends.
Inputs may be any that keep to these rules, and one draw needn't show every extreme that they name: `routes`: in each aligned block of 128 rows no expert is named by more than 64 rows, a bound that some block reaches; the numbers of one row differ.
All inputs are finite; a program needn't handle non-finite values.
Results may differ from the reference program's by a relative error of at most 0.01.
Values may be sent and summed in bfloat16 or wider, within the bound.
No kernel may reach another device: no remote copies, remote signals or barrier semaphores. Data moves between devices by JAX's collectives and lax.ppermute only.
A program may use at most 128 MiB of HBM per device.

```python
import math
import jax
import jax.numpy as jnp
import numpy as np
from jax import lax

D = 2048
FF = 1024
HEADS = 32
DK = 64
TOPK = 2
SPAN = 128
TOK_DEV = 128
TOKENS = 1024
EXPERTS = 8
CAP = 64
HV = 2048
N_SP = 8


def raised(array, stream_key, source, target, shards_of, factor):
    def block_of(dim):
        return (jnp.arange(array.shape[dim]) // (array.shape[dim] // shards_of)).reshape((-1,) + (1,) * (array.ndim - 1 - dim))

    near = jax.random.permutation(stream_key, shards_of)[block_of(target)]
    far = (block_of(target) + shards_of // 2) % shards_of
    return jnp.where((block_of(source) == near) | (block_of(source) == far), factor * array, array)


def block_levels(rng, extent, split, smallest, high):
    level, own = 1.0, jax.random.fold_in(rng, 6)
    for axis_at, parts in split:
        heights = jnp.exp(jax.random.uniform(jax.random.fold_in(own, axis_at), (parts,), jnp.float32, smallest / len(split), high / len(split)))
        level = level * jnp.repeat(heights, extent[axis_at] // parts).reshape([-1 if axis == axis_at else 1 for axis in range(len(extent))])
    return level


def routed_block(rng, own, number, rows, amount, top, limit, lean):
    sequence = jax.random.permutation(rng, amount)
    heavy_load, common = shares(amount, rows * top, limit, lean, True), shares(amount, rows * top, limit, lean, False)
    places = jnp.arange(amount)

    def named(tallies, turn):
        used = int((tallies > 0).sum())
        fixed = max(1, used // 4)
        moved = fixed + (places - fixed + turn * (used - fixed)) % max(1, amount - fixed)
        return jnp.zeros((amount,), jnp.int32).at[sequence[jnp.where(places < fixed, places, moved)]].set(jnp.asarray(tallies, jnp.int32))

    tallies = jnp.where(number % 4 == 0, named(heavy_load, number // 4), named(common, number - number // 4 - 1))
    mixed = jax.random.permutation(jax.random.fold_in(own, 3), amount)
    donor, receiver = mixed[0:amount // 2 * 2:2], mixed[1:amount // 2 * 2:2]
    slack = jnp.minimum(tallies[donor] - 1, limit - tallies[receiver]) // 2
    slack = jnp.where((donor == sequence[0]) | (receiver == sequence[0]) | (tallies[receiver] == 0), 0, jnp.maximum(slack, 0))
    moved = jax.random.randint(jax.random.fold_in(own, 4), (amount // 2,), 0, 1 << 20) % (slack + 1)
    tallies = tallies.at[donor].add(-moved).at[receiver].add(moved)
    members = jnp.searchsorted(jnp.cumsum(tallies), jnp.arange(rows * top), side="right").astype(jnp.int32)
    listing = members.reshape(top, rows).T
    listing = listing[jax.random.permutation(jax.random.fold_in(own, 1), rows)]
    turn = jax.random.randint(jax.random.fold_in(own, 2), (rows, 1), 0, top)
    return jnp.take_along_axis(listing, (jnp.arange(top)[None, :] + turn) % top, axis=1)


def shares(number_of, total, bound, skew, full):
    weights = [(1 << 20) // math.isqrt(grade ** skew) + 1 for grade in range(1, number_of + 1)]
    largest = bound if full else min(bound, max(-(-total // number_of), total * weights[0] // sum(weights)))
    least = 1 if total - largest >= number_of - 1 else 0
    counts, surplus = [largest] + [least] * (number_of - 1), total - largest - least * (number_of - 1)
    while surplus > 0:
        candidates = [i for i in range(1, number_of) if counts[i] < largest] or [i for i in range(1, number_of) if counts[i] < bound]
        whole, left = sum([weights[i] for i in candidates]), surplus
        for i in candidates:
            more = min(bound - counts[i], max(1, left * weights[i] // whole), surplus)
            counts[i] = counts[i] + more
            surplus = surplus - more
    return np.array(counts)


def noise(rng, shape, spread, limit, pieces=(), kind=jnp.bfloat16):
    drawn = jax.random.normal(rng, shape, jnp.float32) * spread
    if len(pieces) > 0:
        drawn = block_levels(rng, shape, pieces, -0.22, 0.18) * drawn
    return jnp.clip(drawn, min=-limit, max=limit).astype(kind)


def bell_draw_with(key, shape, scale, limit, split, heavy, held_as=jnp.bfloat16):
    values = scale * jax.random.normal(key, shape, jnp.float32)
    if split:
        values = values * block_levels(key, shape, split, -0.22, 0.18)
    return jnp.clip(raised(values, jax.random.fold_in(key, 3), *heavy), -limit, limit).astype(held_as)


def setup_inputs(seed: int = 0) -> dict:
    seeds = jax.random.split(jax.random.key(seed), 14)
    layer_input = noise(seeds[0], (TOKENS, D), 1.0, 6.0, ((0, 8),))
    out_cot = bell_draw_with(seeds[1], (TOKENS, D), 1.0, 6.0, ((0, 8),), (0, 1, 8, 2.0))
    routes_keys = jax.random.split(jax.random.fold_in(seeds[2], 1), TOKENS // TOK_DEV)
    routes_turns = jax.random.permutation(jax.random.fold_in(seeds[2], 3), TOKENS // TOK_DEV)
    routes = jax.vmap(lambda own, number: routed_block(jax.random.fold_in(seeds[2], 2), own, number, TOK_DEV, EXPERTS, TOPK, CAP, 1))(routes_keys, routes_turns).reshape((TOKENS, TOPK))
    route_weights = jnp.clip(0.2 + 0.8 * jax.random.uniform(seeds[3], (TOKENS, TOPK), jnp.float32) ** block_levels(seeds[3], (TOKENS, TOPK), ((0, 8),), -0.2, 0.2), 0.2, 1.0)
    gate_weights = noise(seeds[4], (EXPERTS, D, FF), D ** -0.5, 0.125, ((0, 8), (2, 4)))
    up_weights = noise(seeds[5], (EXPERTS, D, FF), D ** -0.5, 0.125, ((0, 8), (2, 4)))
    down_weights = noise(seeds[6], (EXPERTS, FF, D), FF ** -0.5, 0.1875, ((0, 8), (1, 4)))
    out_proj = noise(seeds[7], (D, HV), HV ** -0.5, 0.125, ((1, 4),))
    queries = noise(seeds[8], (TOKENS, HV), 1.0, 6.0, ((0, 8), (1, 4)))
    keys = noise(seeds[9], (TOKENS, HV), 1.0, 6.0, ((0, 8), (1, 4)))
    values = noise(seeds[10], (TOKENS, HV), 1.0, 6.0, ((0, 8), (1, 4)))
    mixer_out = noise(seeds[11], (TOKENS, HV), 1.0, 6.0, ((0, 8), (1, 4)))
    entry_states = noise(seeds[12], (N_SP, HEADS, DK, DK), 1.0, 6.0, ((0, 8), (1, 4)), jnp.float32)
    return dict(layer_input=layer_input, out_cot=out_cot, routes=routes, route_weights=route_weights, gate_weights=gate_weights, up_weights=up_weights, down_weights=down_weights, out_proj=out_proj, queries=queries, keys=keys, values=values, mixer_out=mixer_out, entry_states=entry_states)


def decay_rates(head_ids, head_count, token_count):
    half_count = head_count // 2
    fraction = jnp.minimum(head_ids, half_count) / half_count
    base_rate = jnp.exp((1.0 - fraction) * jnp.log(1.0 / 32.0) + fraction * jnp.log(1.0 / token_count))
    return base_rate * (1.0 + jnp.maximum(head_ids - half_count, 0.0) / half_count)

def position_norm(positions, head_rates):
    return jnp.sqrt(jnp.expm1(-2.0 * head_rates)[None, :] / jnp.expm1(-2.0 * head_rates[None, :] * (positions[:, None] + 1.0)))

def rounded(values):
    return lax.optimization_barrier(values.astype(jnp.bfloat16)).astype(jnp.float32)

def retention_grads(queries, keys, values, head_cot, entry_states, head_rates):
    span_count = TOKENS // SPAN
    per_segment = TOK_DEV // SPAN
    key_scale = DK ** (-0.5)
    span_shape = (span_count, SPAN, HEADS, DK)
    query_wide = queries.reshape(span_shape).astype(jnp.float32)
    key_wide = keys.reshape(span_shape).astype(jnp.float32)
    value_wide = values.reshape(span_shape).astype(jnp.float32)
    cot_wide = head_cot.reshape(span_shape).astype(jnp.float32)
    offsets = jnp.arange(SPAN).astype(jnp.float32)
    distance = offsets[:, None] - offsets[None, :]
    decay_mat = jnp.where(distance[None] >= 0, jnp.exp(-head_rates[:, None, None] * jnp.maximum(distance, 0.0)[None]), 0.0)
    fwd_weights = rounded(jnp.einsum('cihd,cjhd->chij', query_wide, key_wide) * key_scale * decay_mat[None])
    back_weights = rounded(jnp.einsum('cihd,cjhd->chij', cot_wide, value_wide) * decay_mat[None])
    tail_decay = jnp.exp(-head_rates[None, :] * (SPAN - 1.0 - offsets)[:, None])
    lead_decay = jnp.exp(-head_rates[None, :] * (offsets + 1.0)[:, None])
    span_decay = jnp.exp(-head_rates * SPAN)
    updates = key_scale * jnp.einsum('cjhd,cjhe->chde', key_wide * tail_decay[None, :, :, None], value_wide, precision=lax.Precision.HIGHEST)
    backs = jnp.einsum('cihd,cihe->chde', query_wide * lead_decay[None, :, :, None], cot_wide, precision=lax.Precision.HIGHEST)

    def forward(carried, inputs_c):
        update, span_index = inputs_c
        saved_state = entry_states[span_index // per_segment]
        current = jnp.where(span_index % per_segment == 0, saved_state, carried)
        return (span_decay[:, None, None] * current + update, current)
    start_state = jnp.zeros((HEADS, DK, DK), jnp.float32)
    _, fwd_states = lax.scan(forward, start_state, (updates, jnp.arange(span_count, dtype=jnp.int32)))

    def backward(carried, update):
        return (span_decay[:, None, None] * carried + update, carried)
    _, rev_states = lax.scan(backward, start_state, backs, reverse=True)
    grad_q = key_scale * jnp.einsum('chij,cjhd->cihd', back_weights, key_wide)
    grad_q = grad_q + lead_decay[None, :, :, None] * jnp.einsum('chde,cihe->cihd', fwd_states, cot_wide, precision=lax.Precision.HIGHEST)
    grad_k = jnp.einsum('chij,cihd->cjhd', back_weights, query_wide)
    grad_k = key_scale * (grad_k + tail_decay[None, :, :, None] * jnp.einsum('chde,cjhe->cjhd', rev_states, value_wide, precision=lax.Precision.HIGHEST))
    grad_v = jnp.einsum('chij,cihe->cjhe', fwd_weights, cot_wide)
    grad_v = grad_v + key_scale * tail_decay[None, :, :, None] * jnp.einsum('chde,cjhd->cjhe', rev_states, key_wide, precision=lax.Precision.HIGHEST)
    flat_shape = (TOKENS, HEADS * DK)
    return (grad_q.reshape(flat_shape).astype(jnp.bfloat16), grad_k.reshape(flat_shape).astype(jnp.bfloat16), grad_v.reshape(flat_shape).astype(jnp.bfloat16))

def reference(layer_input, out_cot, routes, route_weights, gate_weights, up_weights, down_weights, out_proj, queries, keys, values, mixer_out, entry_states):
    pair_total = TOKENS * TOPK
    per_block = TOK_DEV * TOPK
    slot_count = N_SP * CAP
    flat_routes = routes.reshape(-1)
    onehot = (flat_routes.reshape(N_SP, per_block, 1) == jnp.arange(EXPERTS, dtype=jnp.int32)[None, None, :]).astype(jnp.int32)
    earlier = jnp.cumsum(onehot, axis=1) - onehot
    placed = lax.optimization_barrier(jnp.sum(earlier * onehot, axis=2)).reshape(-1)
    block_id = jnp.arange(pair_total, dtype=jnp.int32) // per_block
    target = flat_routes * slot_count + block_id * CAP + placed
    owner_tok = jnp.arange(pair_total, dtype=jnp.int32) // TOPK
    slot_tok = jnp.full((EXPERTS * slot_count,), TOKENS, jnp.int32).at[target].set(owner_tok)
    slot_weight = jnp.zeros((EXPERTS * slot_count,), jnp.float32).at[target].set(route_weights.reshape(-1))
    blank_row = jnp.zeros((1, D), jnp.bfloat16)
    input_ext = jnp.concatenate([layer_input, blank_row], 0)
    cot_ext = jnp.concatenate([out_cot, blank_row], 0)

    def expert_step(accum, inputs_e):
        gate_w, up_w, down_w, row_ids, row_weight = inputs_e
        exp_rows = input_ext[row_ids]
        exp_cot = (row_weight[:, None] * cot_ext[row_ids].astype(jnp.float32)).astype(jnp.bfloat16)
        gate_pre = jnp.dot(exp_rows, gate_w, preferred_element_type=jnp.float32)
        up_pre = jnp.dot(exp_rows, up_w, preferred_element_type=jnp.float32)
        sigmoid_g = jax.nn.sigmoid(gate_pre)
        activated = (gate_pre * sigmoid_g * up_pre).astype(jnp.bfloat16)
        grad_down = jnp.dot(activated.T, exp_cot, preferred_element_type=jnp.float32).astype(jnp.bfloat16)
        d_act = jnp.dot(exp_cot, down_w.T, preferred_element_type=jnp.float32)
        d_gate = (d_act * up_pre * sigmoid_g * (1.0 + gate_pre * (1.0 - sigmoid_g))).astype(jnp.bfloat16)
        d_up = (d_act * gate_pre * sigmoid_g).astype(jnp.bfloat16)
        grad_gate = jnp.dot(exp_rows.T, d_gate, preferred_element_type=jnp.float32).astype(jnp.bfloat16)
        grad_up = jnp.dot(exp_rows.T, d_up, preferred_element_type=jnp.float32).astype(jnp.bfloat16)
        returned = jnp.dot(d_gate, gate_w.T, preferred_element_type=jnp.float32)
        returned = returned + jnp.dot(d_up, up_w.T, preferred_element_type=jnp.float32)
        return (accum.at[row_ids].add(rounded(returned)), (grad_gate, grad_up, grad_down))
    accum, expert_out = lax.scan(expert_step, jnp.zeros((TOKENS + 1, D), jnp.float32), (gate_weights, up_weights, down_weights, slot_tok.reshape(EXPERTS, slot_count), slot_weight.reshape(EXPERTS, slot_count)))
    grad_gate, grad_up, grad_down = expert_out
    mixer_cot = (out_cot.astype(jnp.float32) + accum[:TOKENS]).astype(jnp.bfloat16)
    grad_proj = jnp.dot(mixer_cot.T, mixer_out, preferred_element_type=jnp.float32)
    head_rates = decay_rates(jnp.arange(HEADS).astype(jnp.float32), HEADS, TOKENS)
    positions = jnp.arange(TOKENS).astype(jnp.float32)
    head_cot = jnp.dot(mixer_cot, out_proj, preferred_element_type=jnp.float32).reshape(TOKENS, HEADS, DK)
    head_cot = (head_cot * position_norm(positions, head_rates)[:, :, None]).astype(jnp.bfloat16)
    grad_q, grad_k, grad_v = retention_grads(queries, keys, values, head_cot, entry_states, head_rates)
    return (grad_gate, grad_up, grad_down, grad_proj, grad_q, grad_k, grad_v)
```

```python
import functools

import jax
import jax.numpy as jnp
from jax import lax
from jax.experimental import pallas as pl
from jax.experimental.pallas import tpu as pltpu
from jax.sharding import PartitionSpec as P

DK = 64
SPAN = 128
F32 = jnp.float32
BF16 = jnp.bfloat16
NN = (((1,), (0,)), ((), ()))
NT = (((1,), (1,)), ((), ()))
TN = (((0,), (0,)), ((), ()))


def dot(a, b, dims=NN, precision=None):
    return lax.dot_general(a, b, dims, precision=precision, preferred_element_type=F32)


def decay_rates(head_ids, head_count, token_count):
    half_count = head_count // 2
    fraction = jnp.minimum(head_ids, half_count) / half_count
    base_rate = jnp.exp(
        (1.0 - fraction) * jnp.log(1.0 / 32.0) + fraction * jnp.log(1.0 / token_count)
    )
    return base_rate * (1.0 + jnp.maximum(head_ids - half_count, 0.0) / half_count)


def position_norm(positions, head_rates):
    return jnp.sqrt(
        jnp.expm1(-2.0 * head_rates)[None, :]
        / jnp.expm1(-2.0 * head_rates[None, :] * (positions[:, None] + 1.0))
    )


def slot_table(routes, experts):
    tokens = routes.shape[0]
    lanes = lax.broadcasted_iota(jnp.int32, (tokens, experts), 1)
    named = jnp.zeros((tokens, experts), F32)
    for k in range(routes.shape[1]):
        named = named + (routes[:, k : k + 1] == lanes).astype(F32)
    row = lax.broadcasted_iota(jnp.int32, (tokens, tokens), 0)
    col = lax.broadcasted_iota(jnp.int32, (tokens, tokens), 1)
    before = (col < row).astype(BF16)
    earlier = dot(before, named.astype(BF16))
    return named * (earlier + 1.0), lanes


def dispatch_kernel(me_ref, routes_ref, weights_ref, rows_ref, cot_ref, out_rows, out_cot, *, experts, share):
    routes = routes_ref[...]
    table, lanes = slot_table(routes, experts)
    picks = experts * share
    tokens = routes.shape[0]
    owner = lax.broadcasted_iota(jnp.int32, (picks, experts), 0) // share
    of_expert = owner == lax.broadcasted_iota(jnp.int32, (picks, experts), 1)
    spread = dot(of_expert.astype(BF16), table.astype(BF16), NT)
    wanted = lax.broadcasted_iota(jnp.int32, (picks, tokens), 0) % share + me_ref[0] * share + 1
    chosen = spread == wanted.astype(F32)
    pick = chosen.astype(BF16)
    weight = jnp.zeros((tokens, experts), F32)
    for k in range(routes.shape[1]):
        weight = weight + jnp.where(routes[:, k : k + 1] == lanes, weights_ref[:, k : k + 1], 0.0)
    slot_weight = jnp.sum(
        jnp.where(of_expert, dot(chosen.astype(F32), weight, precision=lax.Precision.HIGHEST), 0.0),
        axis=1,
        keepdims=True,
    )
    out_rows[...] = dot(pick, rows_ref[...]).astype(BF16)
    out_cot[...] = (slot_weight * dot(pick, cot_ref[...])).astype(BF16)


def combine_kernel(me_ref, routes_ref, cot_ref, back_ref, out_ref, *, experts, share, masks):
    table, _ = slot_table(routes_ref[...], experts)
    capacity = share * len(masks)
    picks = experts * capacity
    place = lax.broadcasted_iota(jnp.int32, (picks, experts), 0)
    of_expert = (place // capacity == lax.broadcasted_iota(jnp.int32, (picks, experts), 1)).astype(BF16)
    spread = dot(table.astype(BF16), of_expert, NT)
    at = lax.broadcasted_iota(jnp.int32, spread.shape, 1) % capacity
    part = at // share
    mask = jnp.zeros_like(part)
    for p, m in enumerate(masks):
        mask = jnp.where(part == p, m, mask)
    wanted = (mask ^ me_ref[0]) * share + at % share + 1
    pick = (spread == wanted.astype(F32)).astype(BF16)
    out_ref[...] = (cot_ref[...].astype(F32) + dot(pick, back_ref[...])).astype(BF16)


def hidden_kernel(*refs, parts):
    row_refs, (gate_ref, up_ref, act_ref, fac_gate, fac_up) = refs[:parts], refs[parts:]
    for p, row_ref in enumerate(row_refs):
        rows = row_ref[...]
        gate_pre = dot(rows, gate_ref[...])
        up_pre = dot(rows, up_ref[...])
        sig = jax.nn.sigmoid(gate_pre)
        silu = gate_pre * sig
        act_ref[p] = (silu * up_pre).astype(BF16)
        fac_gate[p] = up_pre * sig * (1.0 + gate_pre * (1.0 - sig))
        fac_up[p] = silu


def back_kernel(me_ref, *refs, parts, orders):
    cot_refs = refs[:parts]
    down_ref, fac_gate, fac_up, gate_ref, up_ref, dgate_ref, dup_ref = refs[parts : parts + 7]
    outs = refs[parts + 7 :]
    width = gate_ref.shape[0]
    cols = width // parts
    grads = []
    for p in range(parts):
        d_act = dot(cot_refs[p][...], down_ref[...], NT)
        d_gate = (d_act * fac_gate[p]).astype(BF16)
        d_up = (d_act * fac_up[p]).astype(BF16)
        dgate_ref[p] = d_gate
        dup_ref[p] = d_up
        grads.append((d_gate, d_up))
    for out, (mask, order) in zip(outs, orders):
        first = pl.multiple_of((me_ref[0] ^ mask) * cols, cols)
        gate = gate_ref[pl.ds(first, cols), :]
        up = up_ref[pl.ds(first, cols), :]
        for p in range(parts):
            value = dot(grads[p][0], gate, NT) + dot(grads[p][1], up, NT)
            out[order[p]] = value.astype(out.dtype)


def vmem():
    return pl.BlockSpec(memory_space=pltpu.VMEM)


def smem():
    return pl.BlockSpec(memory_space=pltpu.SMEM)


def cost(flops, nbytes):
    return pl.CostEstimate(flops=int(flops), bytes_accessed=int(nbytes), transcendentals=0)


def per_device(
    layer_input,
    out_cot,
    routes,
    route_weights,
    gate_weights,
    up_weights,
    down_weights,
    out_proj,
    queries,
    keys,
    values,
    mixer_out,
    entry_states,
):
    tok_rows, width = layer_input.shape
    experts = lax.axis_size("sp")
    narrow = lax.axis_size("tp")
    here = lax.axis_index("sp")
    me = lax.axis_index("tp")
    me_arr = me.astype(jnp.int32).reshape(1)
    capacity = 2 * tok_rows * routes.shape[1] // experts
    share = capacity // narrow
    picks = experts * share
    cols = width // narrow
    gate_w, up_w, down_w = gate_weights[0], up_weights[0], down_weights[0]
    hidden = gate_w.shape[1]
    bits = [1 << b for b in range(narrow.bit_length() - 1)]

    def swap(value, mask):
        return lax.ppermute(value, "tp", [(i, i ^ mask) for i in range(narrow)])

    def exchange(value):
        return lax.all_to_all(value, "sp", split_axis=0, concat_axis=0, tiled=True)

    part_rows, part_cot = pl.pallas_call(
        functools.partial(dispatch_kernel, experts=experts, share=share),
        out_shape=[jax.ShapeDtypeStruct((picks, width), BF16)] * 2,
        in_specs=[smem(), vmem(), vmem(), vmem(), vmem()],
        out_specs=[vmem(), vmem()],
        name="dispatch",
    )(me_arr, routes, route_weights, layer_input, out_cot)
    got_rows = exchange(part_rows.reshape(experts, share, width)).reshape(picks, width)
    got_cot = exchange(part_cot.reshape(experts, share, width)).reshape(picks, width)

    def spread_over_tp(value):
        found = [value]
        for bit in reversed(bits):
            found = found + [swap(v, bit) for v in found]
        return found

    masks = [0]
    for bit in reversed(bits):
        masks = masks + [m | bit for m in masks]
    rows = spread_over_tp(got_rows)
    cots = spread_over_tp(got_cot)

    act, fac_gate, fac_up = pl.pallas_call(
        functools.partial(hidden_kernel, parts=narrow),
        out_shape=[
            jax.ShapeDtypeStruct((narrow, picks, hidden), BF16),
            jax.ShapeDtypeStruct((narrow, picks, hidden), F32),
            jax.ShapeDtypeStruct((narrow, picks, hidden), F32),
        ],
        in_specs=[vmem()] * (narrow + 2),
        out_specs=[vmem()] * 3,
        cost_estimate=cost(4 * narrow * picks * width * hidden, 6e6),
        name="hidden",
    )(*rows, gate_w, up_w)

    position = {m: p for p, m in enumerate(masks)}
    orders = [(m, [position[masks[p] ^ m] for p in range(narrow)]) for m in range(narrow)]
    back = pl.pallas_call(
        functools.partial(back_kernel, parts=narrow, orders=orders),
        out_shape=[jax.ShapeDtypeStruct((narrow, picks, hidden), BF16)] * 2
        + [jax.ShapeDtypeStruct((narrow, picks, cols), BF16 if m & 1 else F32) for m in range(narrow)],
        in_specs=[smem()] + [vmem()] * (narrow + 5),
        out_specs=[vmem()] * (narrow + 2),
        cost_estimate=cost(6 * narrow * picks * width * hidden, 12e6),
        name="back",
    )(me_arr, *cots, down_w, fac_gate, fac_up, gate_w, up_w)
    d_gate, d_up, partial = back[0], back[1], list(back[2:])
    for bit in bits:
        count = narrow // bit
        for m in reversed(range(0, narrow, 2 * bit)):
            received = swap(partial[m + bit].astype(BF16), bit)
            partial[m] = partial[m].astype(F32) + received.astype(F32)
    returning = (
        partial[0]
        .astype(BF16)
        .reshape(narrow, experts, share, cols)
        .transpose(1, 0, 2, 3)
        .reshape(experts, capacity, cols)
    )
    returned = exchange(returning).reshape(experts * capacity, cols)
    cot_cols = pl.pallas_call(
        functools.partial(combine_kernel, experts=experts, share=share, masks=masks),
        out_shape=jax.ShapeDtypeStruct((tok_rows, cols), BF16),
        grid_spec=pltpu.PrefetchScalarGridSpec(
            num_scalar_prefetch=1,
            grid=(1,),
            in_specs=[
                pl.BlockSpec(routes.shape, lambda i, s: (0, 0)),
                pl.BlockSpec((tok_rows, cols), lambda i, s: (0, s[0])),
                pl.BlockSpec(returned.shape, lambda i, s: (0, 0)),
            ],
            out_specs=pl.BlockSpec((tok_rows, cols), lambda i, s: (0, 0)),
        ),
        name="combine",
    )(me_arr, routes, out_cot, returned)
    mixer_cot = lax.all_gather(cot_cols, "tp", axis=1, tiled=True)

    all_rows = jnp.concatenate(rows, 0)
    all_cots = jnp.concatenate(cots, 0)
    grad_gate = dot(all_rows, d_gate.reshape(-1, hidden), TN).astype(BF16)[None]
    grad_up = dot(all_rows, d_up.reshape(-1, hidden), TN).astype(BF16)[None]
    grad_down = dot(act.reshape(-1, hidden), all_cots, TN).astype(BF16)[None]

    heads = queries.shape[1] // DK
    head_ids = (me * heads + jnp.arange(heads, dtype=jnp.int32)).astype(F32)
    rates = decay_rates(head_ids, heads * narrow, tok_rows * experts)
    positions = (here * tok_rows + jnp.arange(tok_rows, dtype=jnp.int32)).astype(F32)
    norm = jnp.repeat(position_norm(positions, rates), DK, axis=1)
    head_cot = (dot(mixer_cot, out_proj) * norm).astype(BF16)
    split = (tok_rows, heads, DK)
    query, key, value, cot = (x.reshape(split) for x in (queries, keys, values, head_cot))
    scale = DK ** (-0.5)
    offsets = jnp.arange(SPAN, dtype=F32)
    distance = offsets[:, None] - offsets[None, :]
    decay = jnp.where(
        distance[None] >= 0, jnp.exp(-rates[:, None, None] * jnp.maximum(distance, 0.0)[None]), 0.0
    )
    tail = jnp.exp(-rates[None, :] * (SPAN - 1.0 - offsets)[:, None])[:, :, None]
    lead = jnp.exp(-rates[None, :] * (offsets + 1.0)[:, None])[:, :, None]

    def ein(spec, a, b):
        return jnp.einsum(spec, a, b, preferred_element_type=F32)

    local = ein("ihd,ihe->dhe", (query.astype(F32) * lead).astype(BF16), cot)
    sent = jnp.broadcast_to(local.astype(BF16).reshape(1, DK, heads * DK), (experts, DK, heads * DK))
    states = exchange(sent)
    ahead = jnp.arange(experts, dtype=jnp.int32) - here
    steps = jnp.exp(-rates[None, :] * (tok_rows * jnp.maximum(ahead - 1, 0)).astype(F32)[:, None])
    steps = jnp.repeat(jnp.where(ahead[:, None] > 0, steps, 0.0), DK, axis=1)
    reverse = jnp.sum(states.astype(F32) * steps[:, None, :], axis=0).astype(BF16).reshape(DK, heads, DK)

    mixed = mixer_out
    mixed, _ = lax.optimization_barrier((mixer_out, got_cot))
    mixed_all = exchange(jnp.broadcast_to(mixed[None], (experts, *mixed.shape))).reshape(-1, mixed.shape[1])
    cot_slice = lax.all_to_all(mixer_cot, "sp", split_axis=1, concat_axis=0, tiled=True)
    grad_proj = dot(cot_slice, mixed_all, TN)

    fwd = (ein("ihd,jhd->hij", query, key) * scale * decay).astype(BF16)
    bwd = (ein("ihd,jhd->hij", cot, value) * decay).astype(BF16)
    grad_q = scale * ein("hij,jhd->ihd", bwd, key) + lead * ein(
        "hde,ihe->ihd", entry_states[0].astype(BF16), cot
    )
    grad_k = scale * (ein("hij,ihd->jhd", bwd, query) + tail * ein("dhe,jhe->jhd", reverse, value))
    grad_v = ein("hij,ihe->jhe", fwd, cot) + scale * tail * ein("dhe,jhd->jhe", reverse, key)
    flat = (tok_rows, heads * DK)
    return (
        grad_gate,
        grad_up,
        grad_down,
        grad_proj,
        grad_q.reshape(flat).astype(BF16),
        grad_k.reshape(flat).astype(BF16),
        grad_v.reshape(flat).astype(BF16),
    )


def solution(mesh):
    return jax.shard_map(
        per_device,
        mesh=mesh,
        in_specs=(
            P("sp", None),
            P("sp", None),
            P("sp", None),
            P("sp", None),
            P("sp", None, "tp"),
            P("sp", None, "tp"),
            P("sp", "tp", None),
            P(None, "tp"),
            P("sp", "tp"),
            P("sp", "tp"),
            P("sp", "tp"),
            P("sp", "tp"),
            P("sp", "tp", None, None),
        ),
        out_specs=(
            P("sp", None, "tp"),
            P("sp", None, "tp"),
            P("sp", "tp", None),
            P("sp", "tp"),
            P("sp", "tp"),
            P("sp", "tp"),
            P("sp", "tp"),
        ),
        check_vma=False,
    )
```

```python
import functools

import jax
import jax.numpy as jnp
from jax import lax
from jax.experimental import pallas as pl
from jax.experimental.pallas import tpu as pltpu
from jax.sharding import PartitionSpec as P


DK = 64
F32 = jnp.float32
BF16 = jnp.bfloat16
NN = (((1,), (0,)), ((), ()))
NT = (((1,), (1,)), ((), ()))
TN = (((0,), (0,)), ((), ()))


def dot(a, b, dims=NN, precision=None):
    return lax.dot_general(a, b, dims, precision=precision, preferred_element_type=F32)


def decay_rates(head_ids, head_count, token_count):
    half_count = head_count // 2
    fraction = jnp.minimum(head_ids, half_count) / half_count
    base_rate = jnp.exp(
        (1.0 - fraction) * jnp.log(1.0 / 32.0) + fraction * jnp.log(1.0 / token_count)
    )
    return base_rate * (1.0 + jnp.maximum(head_ids - half_count, 0.0) / half_count)


def position_norm(positions, head_rates):
    return jnp.sqrt(
        jnp.expm1(-2.0 * head_rates)[None, :]
        / jnp.expm1(-2.0 * head_rates[None, :] * (positions[:, None] + 1.0))
    )


def slot_table(routes, experts):
    top, tokens = routes.shape
    expert = lax.broadcasted_iota(jnp.int32, (experts, tokens), 0)
    named = jnp.zeros((experts, tokens), F32)
    for k in range(top):
        named = named + (routes[k : k + 1, :] == expert).astype(F32)
    row = lax.broadcasted_iota(jnp.int32, (tokens, tokens), 0)
    col = lax.broadcasted_iota(jnp.int32, (tokens, tokens), 1)
    earlier = dot(named.astype(BF16), (row < col).astype(BF16))
    return named * (earlier + 1.0), expert


def dispatch_kernel(
    me_ref, routes_ref, weights_ref, rows_hbm, cot_hbm, out_rows, out_cot, rows_ref, cot_ref, sems, *, experts, share
):
    copies = [
        pltpu.make_async_copy(rows_hbm, rows_ref, sems.at[0]),
        pltpu.make_async_copy(cot_hbm, cot_ref, sems.at[1]),
    ]
    for copy in copies:
        copy.start()
    routes = routes_ref[...]
    table, expert = slot_table(routes, experts)
    picks = experts * share
    top, tokens = routes.shape
    owner = lax.broadcasted_iota(jnp.int32, (picks, experts), 0) // share
    of_expert = (owner == lax.broadcasted_iota(jnp.int32, (picks, experts), 1)).astype(F32)
    spread = dot(of_expert.astype(BF16), table.astype(BF16))
    wanted = lax.broadcasted_iota(jnp.int32, (picks, tokens), 0) % share + me_ref[0] * share + 1
    chosen = spread == wanted.astype(F32)
    pick = chosen.astype(BF16)
    weight = jnp.zeros((experts, tokens), F32)
    for k in range(top):
        weight = weight + jnp.where(routes[k : k + 1, :] == expert, weights_ref[k : k + 1, :], 0.0)
    wide = dot(of_expert, weight, precision=lax.Precision.HIGHEST)
    slot_weight = jnp.sum(jnp.where(chosen, wide, 0.0), axis=1, keepdims=True)
    copies[0].wait()
    out_rows[...] = dot(pick, rows_ref[...]).astype(BF16)
    copies[1].wait()
    out_cot[...] = (slot_weight * dot(pick, cot_ref[...])).astype(BF16)


def places_kernel(me_ref, routes_ref, out_ref, *, experts, share, masks):
    table, _ = slot_table(routes_ref[...], experts)
    capacity = share * len(masks)
    picks = experts * capacity
    place = lax.broadcasted_iota(jnp.int32, (experts, picks), 1)
    of_expert = place // capacity == lax.broadcasted_iota(jnp.int32, (experts, picks), 0)
    spread = dot(table.astype(BF16), of_expert.astype(BF16), TN)
    at = lax.broadcasted_iota(jnp.int32, spread.shape, 1) % capacity
    part = at // share
    mask = jnp.zeros_like(part)
    for p, m in enumerate(masks):
        mask = jnp.where(part == p, m, mask)
    wanted = (mask ^ me_ref[0]) * share + at % share + 1
    out_ref[...] = (spread == wanted.astype(F32)).astype(BF16)


def hidden_kernel(*refs, parts):
    row_refs, (gate_hbm, up_hbm), (act_ref, fac_gate, fac_up) = refs[:parts], refs[parts : parts + 2], refs[parts + 2 : parts + 5]
    rows_buf, gate_ref, up_ref, sems = refs[parts + 5 :]
    weights = [
        pltpu.make_async_copy(gate_hbm, gate_ref, sems.at[parts]),
        pltpu.make_async_copy(up_hbm, up_ref, sems.at[parts + 1]),
    ]
    copies = [pltpu.make_async_copy(row_refs[p], rows_buf.at[p], sems.at[p]) for p in range(parts)]
    for copy in weights + copies:
        copy.start()
    for copy in weights:
        copy.wait()
    for p in range(parts):
        copies[p].wait()
        rows = rows_buf[p]
        gate_pre = dot(rows, gate_ref[...])
        up_pre = dot(rows, up_ref[...])
        sig = jax.nn.sigmoid(gate_pre)
        silu = gate_pre * sig
        act_ref[p] = (silu * up_pre).astype(BF16)
        fac_gate[p] = up_pre * sig * (1.0 + gate_pre * (1.0 - sig))
        fac_up[p] = silu


def put(out, order, value, parts):
    picks = value.shape[0] // parts
    for p in range(parts):
        piece = value[p * picks : (p + 1) * picks].astype(out.dtype)
        if out.ndim == 4:
            out[:, order[p]] = piece.reshape(out.shape[0], out.shape[2], out.shape[3])
        else:
            out[order[p]] = piece


def first_back_kernel(me_ref, *refs, parts, orders):
    cot_refs = refs[:parts]
    down_hbm, fg_hbm, fu_hbm, gate_hbm, up_hbm, dgate_ref, dup_ref, *outs = refs[parts : parts + 7 + len(orders)]
    cot_buf, down_ref, fac_gate, fac_up, gate_ref, up_ref, sems = refs[parts + 7 + len(orders) :]
    picks = cot_buf.shape[0] // parts
    cols = gate_ref.shape[1]
    copies = [pltpu.make_async_copy(down_hbm, down_ref, sems.at[parts])]
    copies += [pltpu.make_async_copy(cot_refs[p], cot_buf.at[pl.ds(p * picks, picks)], sems.at[p]) for p in range(parts)]
    copies += [
        pltpu.make_async_copy(fg_hbm, fac_gate, sems.at[parts + 1]),
        pltpu.make_async_copy(fu_hbm, fac_up, sems.at[parts + 2]),
    ]
    late = []
    for k, (mask, _) in enumerate(orders):
        first = pl.multiple_of((me_ref[0] ^ mask) * cols, cols)
        late.append(pltpu.make_async_copy(gate_hbm.at[pl.ds(first, cols)], gate_ref.at[k], sems.at[parts + 3 + 2 * k]))
        late.append(pltpu.make_async_copy(up_hbm.at[pl.ds(first, cols)], up_ref.at[k], sems.at[parts + 4 + 2 * k]))
    for copy in copies + late:
        copy.start()
    for copy in copies:
        copy.wait()
    d_act = dot(cot_buf[...], down_ref[...], NT)
    grads = []
    for fac, ref in ((fac_gate, dgate_ref), (fac_up, dup_ref)):
        grad = (d_act * fac[...].reshape(d_act.shape)).astype(BF16)
        ref[...] = grad.reshape(ref.shape)
        grads.append(grad)
    for k, (_, order) in enumerate(orders):
        late[2 * k].wait()
        late[2 * k + 1].wait()
        put(outs[k], order, dot(grads[0], gate_ref[k], NT) + dot(grads[1], up_ref[k], NT), parts)


def other_back_kernel(me_ref, dgate_ref, dup_ref, gate_hbm, up_hbm, *refs, parts, orders):
    outs, (gate_ref, up_ref, sems) = refs[: len(orders)], refs[len(orders) :]
    cols = gate_ref.shape[1]
    late = []
    for k, (mask, _) in enumerate(orders):
        first = pl.multiple_of((me_ref[0] ^ mask) * cols, cols)
        late.append(pltpu.make_async_copy(gate_hbm.at[pl.ds(first, cols)], gate_ref.at[k], sems.at[2 * k]))
        late.append(pltpu.make_async_copy(up_hbm.at[pl.ds(first, cols)], up_ref.at[k], sems.at[2 * k + 1]))
    for copy in late:
        copy.start()
    grads = [ref[...].reshape(-1, ref.shape[2]) for ref in (dgate_ref, dup_ref)]
    for k, (_, order) in enumerate(orders):
        late[2 * k].wait()
        late[2 * k + 1].wait()
        put(outs[k], order, dot(grads[0], gate_ref[k], NT) + dot(grads[1], up_ref[k], NT), parts)


def head(h):
    return slice(h * DK, (h + 1) * DK)


def local_kernel(me_ref, rates_ref, query_ref, cot_ref, mixer_hbm, out_hbm, states, sems, *, heads, half):
    dests, _, _ = out_hbm.shape
    tokens = query_ref.shape[0]
    packed = states.shape[0]
    mine = (me_ref[0] % 2) * half
    copies = []
    for s in range(dests):
        first = pl.multiple_of(s * 2 * half + mine, half)
        copies.append(
            pltpu.make_async_copy(
                mixer_hbm.at[:, pl.ds(first, half)], out_hbm.at[s, pl.ds(packed, tokens), :], sems.at[s]
            )
        )
    for copy in copies:
        copy.start()
    row = lax.broadcasted_iota(jnp.int32, (tokens, DK), 0).astype(F32)
    for h in range(heads):
        lead = jnp.exp(-rates_ref[h] * (row + 1.0))
        decayed = (query_ref[:, head(h)].astype(F32) * lead).astype(BF16)
        state = dot(decayed, cot_ref[:, head(h)], TN)
        states[(h // 2) * DK : (h // 2 + 1) * DK, head(h % 2)] = state.astype(BF16)
    sends = [
        pltpu.make_async_copy(states, out_hbm.at[s, pl.ds(0, packed), :], sems.at[dests + s]) for s in range(dests)
    ]
    for copy in sends:
        copy.start()
    for copy in copies + sends:
        copy.wait()


def inner_kernel(rates_ref, query_ref, key_ref, value_ref, cot_ref, entry_ref, gq_ref, gk_ref, gv_ref, *, heads):
    tokens = query_ref.shape[0]
    scale = DK ** (-0.5)
    gap = (
        lax.broadcasted_iota(jnp.int32, (tokens, tokens), 0) - lax.broadcasted_iota(jnp.int32, (tokens, tokens), 1)
    ).astype(F32)
    row = lax.broadcasted_iota(jnp.int32, (tokens, DK), 0).astype(F32)
    for h in range(heads):
        rate = rates_ref[h]
        decay = jnp.where(gap >= 0.0, jnp.exp(-rate * jnp.maximum(gap, 0.0)), 0.0)
        query, key, value, cot = (ref[:, head(h)] for ref in (query_ref, key_ref, value_ref, cot_ref))
        fwd = (dot(query, key, NT) * scale * decay).astype(BF16)
        bwd = (dot(cot, value, NT) * decay).astype(BF16)
        lead = jnp.exp(-rate * (row + 1.0))
        gq = scale * dot(bwd, key) + lead * dot(cot, entry_ref[0, h].astype(BF16), NT)
        gq_ref[:, head(h)] = gq.astype(BF16)
        gk_ref[:, head(h)] = scale * dot(bwd, query, TN)
        gv_ref[:, head(h)] = dot(fwd, cot, TN)


def final_kernel(here_ref, rates_ref, key_ref, value_ref, gk_part, gv_part, got_hbm, gk_ref, gv_ref, states, sem, *, heads):
    devices, packed, lanes = states.shape
    copy = pltpu.make_async_copy(got_hbm.at[:, pl.ds(0, packed), :], states, sem)
    copy.start()
    tokens = key_ref.shape[0]
    scale = DK ** (-0.5)
    lane = lax.broadcasted_iota(jnp.int32, (1, lanes), 1)
    row = lax.broadcasted_iota(jnp.int32, (tokens, DK), 0).astype(F32)
    copy.wait()
    for g in range(heads // 2):
        rate = jnp.where(lane < DK, rates_ref[2 * g], rates_ref[2 * g + 1])

        def add(s, total):
            ahead = s - here_ref[0]
            far = (tokens * jnp.maximum(ahead - 1, 0)).astype(F32)
            step = jnp.where(ahead > 0, jnp.exp(-rate * far), 0.0)
            return total + step * states[s, g * DK : (g + 1) * DK, :].astype(F32)

        reverse = lax.fori_loop(0, devices, add, jnp.zeros((DK, lanes), F32), unroll=devices <= 8).astype(BF16)
        for q in range(2):
            h = 2 * g + q
            tail = scale * jnp.exp(-rates_ref[h] * (tokens - 1.0 - row))
            state = reverse[:, head(q)]
            gk_ref[:, head(h)] = (gk_part[:, head(h)] + tail * dot(value_ref[:, head(h)], state, NT)).astype(BF16)
            gv_ref[:, head(h)] = (gv_part[:, head(h)] + tail * dot(key_ref[:, head(h)], state)).astype(BF16)


def proj_kernel(me_ref, mine_hbm, other_ref, mixed_ref, out_ref, mine_ref, sem):
    devices, tokens, half = mine_ref.shape
    copy = pltpu.make_async_copy(mine_hbm.at[:, pl.ds(mine_hbm.shape[1] - tokens, tokens), :], mine_ref, sem)
    copy.start()
    mixed = mixed_ref[...].reshape(devices * tokens, -1)
    side = me_ref[0] % 2
    out_ref[pl.ds(pl.multiple_of((1 - side) * half, half), half), :] = dot(
        other_ref[...].reshape(devices * tokens, half), mixed, TN
    )
    copy.wait()
    out_ref[pl.ds(pl.multiple_of(side * half, half), half), :] = dot(
        mine_ref[...].reshape(devices * tokens, half), mixed, TN
    )


def vmem():
    return pl.BlockSpec(memory_space=pltpu.VMEM)


def smem():
    return pl.BlockSpec(memory_space=pltpu.SMEM)


def anywhere():
    return pl.BlockSpec(memory_space=pl.ANY)


def sds(shape, dtype):
    return jax.ShapeDtypeStruct(tuple(shape), dtype)


def cost(flops, nbytes):
    return pl.CostEstimate(flops=int(flops), bytes_accessed=int(nbytes), transcendentals=0)


def per_device(
    layer_input,
    out_cot,
    routes,
    route_weights,
    gate_weights,
    up_weights,
    down_weights,
    out_proj,
    queries,
    keys,
    values,
    mixer_out,
    entry_states,
):
    tok_rows, width = layer_input.shape
    experts = lax.axis_size("sp")
    narrow = lax.axis_size("tp")
    here = lax.axis_index("sp")
    me = lax.axis_index("tp")
    me_arr = me.astype(jnp.int32).reshape(1)
    here_arr = here.astype(jnp.int32).reshape(1)
    capacity = 2 * tok_rows * routes.shape[1] // experts
    share = capacity // narrow
    picks = experts * share
    cols = width // narrow
    gate_w, up_w, down_w = gate_weights[0], up_weights[0], down_weights[0]
    hidden = gate_w.shape[1]
    bits = [1 << b for b in range(narrow.bit_length() - 1)]
    routes_t = routes.T
    sems = pltpu.SemaphoreType.DMA

    def swap(value, mask):
        return lax.ppermute(value, "tp", [(i, i ^ mask) for i in range(narrow)])

    def exchange(value):
        return lax.all_to_all(value, "sp", split_axis=0, concat_axis=0, tiled=True)

    part_rows, part_cot = pl.pallas_call(
        functools.partial(dispatch_kernel, experts=experts, share=share),
        out_shape=[sds((picks, width), BF16)] * 2,
        in_specs=[smem(), vmem(), vmem(), anywhere(), anywhere()],
        out_specs=[vmem(), vmem()],
        scratch_shapes=[pltpu.VMEM((tok_rows, width), BF16)] * 2 + [sems((2,))],
        name="dispatch",
    )(me_arr, routes_t, route_weights.T, layer_input, out_cot)
    got_rows = exchange(part_rows.reshape(experts, share, width)).reshape(picks, width)
    got_cot = exchange(part_cot.reshape(experts, share, width)).reshape(picks, width)

    def spread_over_tp(value):
        found = [value]
        for bit in reversed(bits):
            found = found + [swap(v, bit) for v in found]
        return found

    masks = [0]
    for bit in reversed(bits):
        masks = masks + [m | bit for m in masks]
    rows = spread_over_tp(got_rows)
    cots = spread_over_tp(got_cot)

    act, fac_gate, fac_up = pl.pallas_call(
        functools.partial(hidden_kernel, parts=narrow),
        out_shape=[
            sds((narrow, picks, hidden), BF16),
            sds((narrow, picks, hidden), F32),
            sds((narrow, picks, hidden), F32),
        ],
        in_specs=[anywhere()] * (narrow + 2),
        out_specs=[vmem()] * 3,
        scratch_shapes=[pltpu.VMEM((narrow, picks, width), BF16)]
        + [pltpu.VMEM((width, hidden), BF16)] * 2
        + [sems((narrow + 2,))],
        cost_estimate=cost(4 * narrow * picks * width * hidden, 6e6),
        name="hidden",
    )(*rows, gate_w, up_w)

    mixed, _ = lax.optimization_barrier((mixer_out, got_cot))
    mixed_all = exchange(jnp.broadcast_to(mixed[None], (experts, *mixed.shape)))

    position = {m: p for p, m in enumerate(masks)}
    orders = [(m, [position[masks[p] ^ m] for p in range(narrow)]) for m in range(narrow)]
    blocks = (experts, narrow, share, cols) if share % 16 == 0 else (narrow, picks, cols)
    half_count = narrow // 2
    early = [orders[m] for m in reversed(range(half_count, narrow))]
    later = [orders[m] for m in reversed(range(half_count))]
    back = pl.pallas_call(
        functools.partial(first_back_kernel, parts=narrow, orders=early),
        out_shape=[sds((narrow, picks, hidden), BF16)] * 2 + [sds(blocks, BF16)] * len(early),
        in_specs=[smem()] + [anywhere()] * (narrow + 5),
        out_specs=[vmem()] * (2 + len(early)),
        scratch_shapes=[
            pltpu.VMEM((narrow * picks, width), BF16),
            pltpu.VMEM((hidden, width), BF16),
            pltpu.VMEM((narrow, picks, hidden), F32),
            pltpu.VMEM((narrow, picks, hidden), F32),
            pltpu.VMEM((len(early), cols, hidden), BF16),
            pltpu.VMEM((len(early), cols, hidden), BF16),
            sems((narrow + 3 + 2 * len(early),)),
        ],
        cost_estimate=cost(4 * narrow * picks * width * hidden, 9e6),
        name="back",
    )(me_arr, *cots, down_w, fac_gate, fac_up, gate_w, up_w)
    d_gate, d_up = back[:2]
    rest = pl.pallas_call(
        functools.partial(other_back_kernel, parts=narrow, orders=later),
        out_shape=[sds(blocks, BF16)] * len(later),
        in_specs=[smem(), vmem(), vmem(), anywhere(), anywhere()],
        out_specs=[vmem()] * len(later),
        scratch_shapes=[pltpu.VMEM((len(later), cols, hidden), BF16)] * 2 + [sems((2 * len(later),))],
        cost_estimate=cost(2 * narrow * picks * width * hidden, 4e6),
        name="back_rest",
    )(me_arr, d_gate, d_up, gate_w, up_w)
    partial = (list(back[2:]) + list(rest))[::-1]
    for bit in bits:
        for m in reversed(range(0, narrow, 2 * bit)):
            received = swap(partial[m + bit], bit)
            partial[m] = (partial[m].astype(F32) + received.astype(F32)).astype(BF16)
    returning = partial[0]
    if returning.ndim == 3:
        returning = returning.reshape(narrow, experts, share, cols).transpose(1, 0, 2, 3)
    returning, mixed_all = lax.optimization_barrier((returning, mixed_all))
    returned = exchange(returning.reshape(experts, capacity, cols)).reshape(experts * capacity, cols)
    places = pl.pallas_call(
        functools.partial(places_kernel, experts=experts, share=share, masks=masks),
        out_shape=sds((tok_rows, experts * capacity), BF16),
        in_specs=[smem(), vmem()],
        out_specs=vmem(),
        name="places",
    )(me_arr, routes_t)
    own_cols = lax.dynamic_slice_in_dim(out_cot, me * cols, cols, 1)
    cot_cols = (own_cols.astype(F32) + dot(places, returned)).astype(BF16)
    mixer_cot = lax.all_gather(cot_cols, "tp", axis=1, tiled=True)

    all_rows = jnp.concatenate(rows, 0)
    grad_gate = dot(all_rows, d_gate.reshape(-1, hidden), TN).astype(BF16)[None]
    grad_up = dot(all_rows, d_up.reshape(-1, hidden), TN).astype(BF16)[None]
    all_cots = jnp.concatenate(cots, 0)
    grad_down = dot(act.reshape(-1, hidden), all_cots, TN).astype(BF16)[None]

    channels = queries.shape[1]
    heads = channels // DK
    head_ids = (me * heads + jnp.arange(heads, dtype=jnp.int32)).astype(F32)
    rates = decay_rates(head_ids, heads * narrow, tok_rows * experts)
    positions = (here * tok_rows + jnp.arange(tok_rows, dtype=jnp.int32)).astype(F32)
    norm = jnp.repeat(position_norm(positions, rates), DK, axis=1)
    head_cot = (dot(mixer_cot, out_proj) * norm).astype(BF16)
    packed = heads // 2 * DK
    half = width // experts // 2
    flat = (tok_rows, channels)
    if half == 2 * DK:
        sent = pl.pallas_call(
            functools.partial(local_kernel, heads=heads, half=half),
            out_shape=sds((experts, packed + tok_rows, 2 * DK), BF16),
            in_specs=[smem(), smem(), vmem(), vmem(), anywhere()],
            out_specs=anywhere(),
            scratch_shapes=[pltpu.VMEM((packed, 2 * DK), BF16), sems((2 * experts,))],
            name="local",
        )(me_arr, rates, queries, head_cot, mixer_cot)
        got = exchange(sent)
        other = swap(got[:, packed:], 1)
        grad_proj = pl.pallas_call(
            proj_kernel,
            out_shape=sds((2 * half, channels), F32),
            in_specs=[smem(), anywhere(), vmem(), vmem()],
            out_specs=vmem(),
            scratch_shapes=[pltpu.VMEM((experts, tok_rows, half), BF16), sems],
            name="proj",
        )(me_arr, got, other, mixed_all)
    else:
        row = jnp.arange(tok_rows, dtype=F32)[:, None, None]
        lead = jnp.exp(-rates[None, :, None] * (row + 1.0))
        decayed = (queries.reshape(tok_rows, heads, DK).astype(F32) * lead).astype(BF16)
        state = jnp.einsum(
            "ighd,ighe->gdhe",
            decayed.reshape(tok_rows, heads // 2, 2, DK),
            head_cot.reshape(tok_rows, heads // 2, 2, DK),
            preferred_element_type=F32,
        )
        state = state.astype(BF16).reshape(1, packed, 2 * DK)
        got = exchange(jnp.broadcast_to(state, (experts, packed, 2 * DK)))
        slices = lax.all_to_all(mixer_cot, "sp", split_axis=1, concat_axis=0, tiled=True)
        grad_proj = dot(slices, mixed_all.reshape(-1, channels), TN)
    grad_q, gk_part, gv_part = pl.pallas_call(
        functools.partial(inner_kernel, heads=heads),
        out_shape=[sds(flat, BF16), sds(flat, F32), sds(flat, F32)],
        in_specs=[smem()] + [vmem()] * 5,
        out_specs=[vmem()] * 3,
        cost_estimate=cost(heads * 5 * 2 * tok_rows * tok_rows * DK, 2e6),
        name="inner",
    )(rates, queries, keys, values, head_cot, entry_states)
    grad_k, grad_v = pl.pallas_call(
        functools.partial(final_kernel, heads=heads),
        out_shape=[sds(flat, BF16)] * 2,
        in_specs=[smem(), smem()] + [vmem()] * 4 + [anywhere()],
        out_specs=[vmem()] * 2,
        scratch_shapes=[pltpu.VMEM((experts, packed, 2 * DK), BF16), sems],
        name="final",
    )(here_arr, rates, keys, values, gk_part, gv_part, got)
    return grad_gate, grad_up, grad_down, grad_proj, grad_q, grad_k, grad_v


def solution(mesh):
    return jax.shard_map(
        per_device,
        mesh=mesh,
        in_specs=(
            P("sp", None),
            P("sp", None),
            P("sp", None),
            P("sp", None),
            P("sp", None, "tp"),
            P("sp", None, "tp"),
            P("sp", "tp", None),
            P(None, "tp"),
            P("sp", "tp"),
            P("sp", "tp"),
            P("sp", "tp"),
            P("sp", "tp"),
            P("sp", "tp", None, None),
        ),
        out_specs=(
            P("sp", None, "tp"),
            P("sp", None, "tp"),
            P("sp", "tp", None),
            P("sp", "tp"),
            P("sp", "tp"),
            P("sp", "tp"),
            P("sp", "tp"),
        ),
        check_vma=False,
    )
```
